32 devices in a mesh: sp: 8 (over z, x), tp: 4 (over y, core).
Axes of the slice: x: 2, y: 2, z: 4, core: 2. Of those that a mesh axis runs over, the one named last changes fastest.
Arguments:
- tokens_in: bfloat16 [6144, 2048], P(('sp', 'tp')), may hold values from -300 to 300
- norm_gain: float32 [2048], replicated, may hold values from 0.1 to 1.9
- query_weight: bfloat16 [2048, 1024], P('sp', 'tp'), may hold values from -64 to 64
- key_weight: bfloat16 [2048, 512], P('sp', 'tp'), may hold values from -1 to 1
- value_weight: bfloat16 [2048, 512], P('sp', 'tp'), may hold values from -0.125 to 0.125
- pool_weight: bfloat16 [2048, 1024], P('sp', 'tp'), may hold values from -0.125 to 0.125
- sink_logit: float32 [16], P('tp'), may hold values from 1 to 5
- pool_gain: float32 [1024], P('tp'), may hold values from 0.1 to 1.9
- attention_out_weight: bfloat16 [1024, 2048], P('tp', 'sp'), may hold values from -0.125 to 0.125
- pool_out_weight: bfloat16 [1024, 2048], P('tp', 'sp'), may hold values from -0.1875 to 0.1875
Outputs:
- mixed_out: bfloat16 [6144, 2048], P(('sp', 'tp'))
The draws below stay inside these ranges and needn't reach their ends.
All inputs are finite; a program needn't handle non-finite values.
Results may differ from the reference program's by a relative error of at most 0.014.
Values may be sent and summed in bfloat16 or wider, within the bound.
A program may use at most 64 MiB of HBM per device.

```python
import jax
import jax.numpy as jnp
from jax import lax

D = 2048
HEADS = 16
KV_HEADS = 8
HEAD_DIM = 64
POOL_CH = 256
POOL_GROUPS = 4
WINDOW = 128
TOK_DEV = 768
TOKENS = 6144
Q_WIDTH = 1024
KV_WIDTH = 512
POOL_WIDTH = 1024
N_TP = 4


def draw_tokens_in(key, part):
    noise_key = jax.random.fold_in(key, 11)
    direction_key = jax.random.fold_in(key, 12)
    level_key = jax.random.fold_in(key, 13)
    rough = jax.random.normal(noise_key, (TOKENS, D), jnp.float32)
    direction = jax.random.normal(direction_key, (D,), jnp.float32)
    block_count = TOKENS // TOK_DEV
    block_number = jnp.arange(block_count)
    ramp = block_number.astype(jnp.float32) / max(block_count - 1, 1)
    alternate = (1 - 2 * (block_number % 2)).astype(jnp.float32)
    jitter = jax.random.uniform(level_key, (block_count,), jnp.float32, 0.8, 1.3)
    levels = 2.0 * 3.0 ** ramp * jitter * alternate
    level_rows = jnp.repeat(levels, TOK_DEV)
    values = rough + level_rows[:, None] * direction[None, :]
    return jnp.clip(values, -300.0, 300.0).astype(jnp.bfloat16)


def key_base(key):
    limit = 6.0 * D ** (-0.5)
    base = jax.random.normal(jax.random.fold_in(key, 71), (D, KV_HEADS * HEAD_DIM), jnp.float32) * D ** (-0.5)
    base = jnp.clip(base, -limit, limit)
    return base


def draw_key_weight(key, part):
    return jnp.clip(key_base(key), -1.0, 1.0).astype(jnp.bfloat16)


def draw_query_weight(key, part):
    limit = 6.0 * D ** (-0.5)
    own = jax.random.normal(jax.random.fold_in(key, 72), (D, HEADS * HEAD_DIM), jnp.float32) * D ** (-0.5)
    own = jnp.clip(own, -limit, limit)
    return jnp.clip(own, -64.0, 64.0).astype(jnp.bfloat16)


def with_spikes(values, key, source, target, blocks, factor):
    owner, partner = [(jnp.arange(values.shape[dim]) // (values.shape[dim] // blocks)).reshape([-1 if axis == dim else 1 for axis in range(values.ndim)]) for dim in (source, target)]
    chosen = jax.random.permutation(key, blocks)[partner]
    strong = (owner == chosen) | (owner == (partner + blocks // 2) % blocks)
    return jnp.where(strong, factor * values, values)


def level_of(key, shape, split, low, largest):
    level = 1.0
    for dim, shards_of in split:
        steps = jax.random.uniform(jax.random.fold_in(jax.random.fold_in(key, 6), dim), (shards_of,), jnp.float32, low / len(split), largest / len(split))
        level = level * jnp.repeat(jnp.exp(steps), shape[dim] // shards_of).reshape((-1,) + (1,) * (len(shape) - 1 - dim))
    return level


def bell_draw(stream_key, dims, deviation, most, pieces=(), held_as=jnp.bfloat16):
    drawn = deviation * jax.random.normal(stream_key, dims, jnp.float32)
    if pieces:
        drawn = drawn * level_of(stream_key, dims, pieces, -0.22, 0.18)
    return jnp.clip(drawn, -most, most).astype(held_as)


def bell_draw_with(rng, dims, deviation, bound, shards, heavy, dtype=jnp.bfloat16):
    drawn = deviation * jax.random.normal(rng, dims, jnp.float32)
    if shards:
        drawn = drawn * level_of(rng, dims, shards, -0.22, 0.18)
    return jnp.clip(with_spikes(drawn, jax.random.fold_in(rng, 3), *heavy), -bound, bound).astype(dtype)


def setup_inputs(seed: int = 0) -> dict:
    keys = jax.random.split(jax.random.key(seed), 11)
    return {
        "tokens_in": draw_tokens_in(jax.random.fold_in(keys[10], 71), 0),
        "norm_gain": jnp.clip(1.0 + 0.18 * jax.random.normal(keys[1], (D,), jnp.float32), 0.1, 1.9),
        "query_weight": draw_query_weight(jax.random.fold_in(keys[10], 71), 0),
        "key_weight": draw_key_weight(jax.random.fold_in(keys[10], 71), 0),
        "value_weight": bell_draw(keys[4], (D, KV_WIDTH), D ** -0.5, 0.125, ((0, 8), (1, 4))),
        "pool_weight": bell_draw(keys[5], (D, POOL_WIDTH), D ** -0.5, 0.125, ((0, 8), (1, 4))),
        "sink_logit": jnp.clip(1.0 + 4.0 * jax.random.uniform(keys[6], (HEADS,), jnp.float32) ** level_of(keys[6], (HEADS,), ((0, 4),), -0.2, 0.2), 1.0, 5.0),
        "pool_gain": jnp.clip(1.0 + 0.18 * jax.random.normal(keys[7], (POOL_WIDTH,), jnp.float32), 0.1, 1.9),
        "attention_out_weight": bell_draw(keys[8], (Q_WIDTH, D), (Q_WIDTH + POOL_WIDTH) ** -0.5, 0.125, ((0, 4), (1, 8))),
        "pool_out_weight": bell_draw_with(keys[9], (POOL_WIDTH, D), (Q_WIDTH + POOL_WIDTH) ** -0.5, 0.1875, ((0, 4), (1, 8)), (0, 1, 8, 2.0)),
    }


EPS = 1e-06
SHORT_REACHES = (8, 32)

def attention_mix(query_rows, key_rows, value_rows, sink_logit):
    total_rows = query_rows.shape[0]
    blocks = total_rows // WINDOW
    group = HEADS // KV_HEADS
    queries = query_rows.astype(jnp.float32).reshape(blocks, WINDOW, KV_HEADS, group, HEAD_DIM)
    key_blocks = key_rows.astype(jnp.float32).reshape(blocks, WINDOW, KV_HEADS, HEAD_DIM)
    value_blocks = value_rows.astype(jnp.float32).reshape(blocks, WINDOW, KV_HEADS, HEAD_DIM)

    def with_previous(blocks_in):
        earlier = jnp.concatenate([jnp.zeros_like(blocks_in[:1]), blocks_in[:-1]], axis=0)
        return jnp.concatenate([earlier, blocks_in], axis=1)
    key_pairs = with_previous(key_blocks)
    value_pairs = with_previous(value_blocks)
    scores = jnp.einsum('nqhgd,nkhd->nhgqk', queries, key_pairs) * HEAD_DIM ** (-0.5)
    q_index = jnp.arange(WINDOW)[:, None]
    k_index = jnp.arange(2 * WINDOW)[None, :]
    distance = q_index + WINDOW - k_index
    inside = (distance >= 0) & (distance < WINDOW)
    block_index = jnp.arange(blocks)[:, None, None]
    allowed = inside[None] & ((block_index > 0) | (k_index >= WINDOW)[None])
    scores = jnp.where(allowed[:, None, None], scores, -jnp.inf)
    sinks = sink_logit.astype(jnp.float32).reshape(1, KV_HEADS, group, 1, 1)
    peak = jnp.maximum(lax.optimization_barrier(jnp.max(scores, axis=-1, keepdims=True)), sinks)
    expo = jnp.exp(scores - peak)
    denom = lax.optimization_barrier(jnp.sum(expo, axis=-1, keepdims=True)) + jnp.exp(sinks - peak)
    probs = lax.optimization_barrier((expo / denom).astype(jnp.bfloat16))
    attended = jnp.einsum('nhgqk,nkhd->nqhgd', probs.astype(jnp.float32), value_pairs)
    return attended.astype(jnp.bfloat16).reshape(total_rows, HEADS * HEAD_DIM)

def pool_mix(pool_rows, pool_gain):
    total_rows = pool_rows.shape[0]
    values = pool_rows.astype(jnp.float32)
    running = jnp.concatenate([jnp.zeros((1, values.shape[1]), jnp.float32), jnp.cumsum(values, axis=0)], axis=0)
    position = jnp.arange(total_rows)
    outputs = []
    for group_index, reach in enumerate(SHORT_REACHES + (WINDOW,)):
        span = running[:, group_index * POOL_CH:(group_index + 1) * POOL_CH]
        lower = span[jnp.maximum(position + 1 - reach, 0)]
        count = jnp.minimum(position + 1, reach).astype(jnp.float32)[:, None]
        outputs.append((span[1:] - lower) / count)
    whole_prefix = running[1:, (POOL_GROUPS - 1) * POOL_CH:] / (position + 1).astype(jnp.float32)[:, None]
    pooled = jnp.concatenate(outputs + [whole_prefix], axis=1)
    return ((pooled - values) * pool_gain.astype(jnp.float32)).astype(jnp.bfloat16)

def reference(tokens_in, norm_gain, query_weight, key_weight, value_weight, pool_weight, sink_logit, pool_gain, attention_out_weight, pool_out_weight):
    widened = tokens_in.astype(jnp.float32)
    inverse = lax.rsqrt(lax.optimization_barrier(jnp.mean(widened * widened, axis=1, keepdims=True)) + EPS)
    normed = (widened * inverse * norm_gain.astype(jnp.float32)).astype(jnp.bfloat16)
    query_rows = jnp.dot(normed, query_weight, preferred_element_type=jnp.float32).astype(jnp.bfloat16)
    key_rows = jnp.dot(normed, key_weight, preferred_element_type=jnp.float32).astype(jnp.bfloat16)
    value_rows = jnp.dot(normed, value_weight, preferred_element_type=jnp.float32).astype(jnp.bfloat16)
    pool_rows = jnp.dot(normed, pool_weight, preferred_element_type=jnp.float32).astype(jnp.bfloat16)
    attended = attention_mix(query_rows, key_rows, value_rows, sink_logit)
    pool_mixed = pool_mix(pool_rows, pool_gain)
    attend_cols = Q_WIDTH // N_TP
    pool_cols = POOL_WIDTH // N_TP
    summed = jnp.zeros((tokens_in.shape[0], D), jnp.float32)
    for block in range(N_TP):
        partial_sum = jnp.dot(attended[:, block * attend_cols:(block + 1) * attend_cols], attention_out_weight[block * attend_cols:(block + 1) * attend_cols], preferred_element_type=jnp.float32)
        partial_sum = partial_sum + jnp.dot(pool_mixed[:, block * pool_cols:(block + 1) * pool_cols], pool_out_weight[block * pool_cols:(block + 1) * pool_cols], preferred_element_type=jnp.float32)
        rounded = lax.optimization_barrier(partial_sum.astype(jnp.bfloat16))
        summed = summed + rounded.astype(jnp.float32)
    return summed.astype(jnp.bfloat16)
```

```python
import functools
import math

import jax
import jax.numpy as jnp
from jax import lax
from jax.experimental import pallas as pl
from jax.experimental.pallas import tpu as pltpu
from jax.sharding import PartitionSpec as P

HEAD_DIM = 64
POOL_CH = 256
POOL_GROUPS = 4
WINDOW = 128
EPS = 1e-06
SHORT_REACHES = (8, 32)
CORES = 2
SIDE_SHARE = 6
MESH = pl.DeviceIdType.MESH
F32 = jnp.float32
BF16 = jnp.bfloat16


def row_tile(rows, most):
    tile = most
    while rows % tile:
        tile -= 16
    return tile


def kernel(n_sp, n_tp, cols, n_in, n_out, widths, *refs):
    tok, gain, sink, pgain = refs[:4]
    win_refs = refs[4 : 4 + n_in]
    wout_refs = refs[4 + n_in : 4 + n_in + n_out]
    (
        out, xs, wi, wo, acc, ext, mix, tot, carry, dsend, drecv, ysend, yrecv, own,
        local_sem, send_sem, sem_in, sem_in_side, sem_out, sem_out_side,
        sem_tok, sem_halo, sem_tot, sem_core, sem_y,
    ) = refs[4 + n_in + n_out :]
    qw, kw, vw, pw = widths
    levels = n_sp // cols
    chips = n_tp // CORES
    rows, seq = tok.shape[0], xs.shape[1]
    piece = xs.shape[2]
    blocks = seq // WINDOW
    me, t = lax.axis_index("sp"), lax.axis_index("tp")
    z, x = me // cols, me % cols
    y, c = t // CORES, t % CORES
    partner = y * CORES + (1 - c)

    locals_ = []
    at = 0
    for i, ref in enumerate(win_refs):
        w = ref.shape[1]
        locals_.append(pltpu.make_async_copy(ref, wi.at[me, :, pl.ds(at, w)], local_sem.at[i]))
        at += w
    at = 0
    for i, ref in enumerate(wout_refs):
        k = ref.shape[0]
        locals_.append(
            pltpu.make_async_copy(ref, wo.at[me, pl.ds(at, k), :], local_sem.at[n_in + i])
        )
        at += k
    for copy in locals_:
        copy.start()

    barrier = pltpu.get_barrier_semaphore()
    for d in range(1, n_sp):
        pl.semaphore_signal(barrier, inc=1, device_id=((me + d) % n_sp, t), device_id_type=MESH)
    for d in range(1, n_tp):
        pl.semaphore_signal(barrier, inc=1, device_id=(me, (t + d) % n_tp), device_id_type=MESH)
    pl.semaphore_wait(barrier, n_sp + n_tp - 2)

    sent = []

    def when(cond, fn):
        if cond is None:
            fn()
        else:
            pl.when(cond)(fn)

    def both(a, b):
        return b if a is None else (a if b is None else jnp.logical_and(a, b))

    def send(cond, src, dst, recv, dev):
        copy = pltpu.make_async_remote_copy(
            src_ref=src, dst_ref=dst, send_sem=send_sem.at[len(sent)], recv_sem=recv,
            device_id=dev, device_id_type=MESH,
        )
        when(cond, copy.start)
        sent.append((cond, copy))

    def arrived(cond, dst, recv):
        copy = pltpu.make_async_remote_copy(
            src_ref=dst, dst_ref=dst, send_sem=send_sem.at[0], recv_sem=recv,
            device_id=(me, partner), device_id_type=MESH,
        )
        when(cond, copy.wait_recv)

    up, down = z + 1 < levels, z > 0

    class Spread:
        def __init__(self, buf, main_sem, side_sem):
            self.buf, self.main_sem, self.side_sem = buf, main_sem, side_sem
            k = buf.shape[1]
            self.side = max(16, k // SIDE_SHARE // 16 * 16)
            self.main = k - self.side

        def part(self, s, which):
            if which == "all":
                return self.buf.at[s]
            if which == "main":
                return self.buf.at[s, pl.ds(0, self.main), :]
            return self.buf.at[s, pl.ds(self.main, self.side), :]

        def go(self, cond, s, which, dev_sp):
            sem = self.side_sem if which == "side" else self.main_sem
            ref = self.part(s, which)
            send(cond, ref, ref, sem.at[s], (dev_sp, t))

        def across(self, cond, s, which):
            for d in range(1, cols):
                self.go(cond, s, which, z * cols + (x + d) % cols)

        def peers(self, level):
            return [level * cols + (x + cols - d) % cols for d in range(1, cols)]

        def begin(self):
            self.across(None, me, "side")
            self.go(up, me, "all", me + cols)
            self.go(down, me, "all", me - cols)
            self.across(None, me, "main")

        def begin_side(self):
            for s in self.peers(z):
                arrived(None, self.part(s, "side"), self.side_sem.at[s])
                self.go(up, s, "side", me + cols)
                self.go(down, s, "side", me - cols)

        def hop(self, h):
            for level, there, on, to in (
                (z - h, z - h >= 0, up, me + cols),
                (z + h, z + h < levels, down, me - cols),
            ):
                s = level * cols + x
                arrived(there, self.part(s, "all"), self.main_sem.at[s])
                self.go(both(there, on), s, "all", to)
                self.across(there, s, "main")
                for s in self.peers(level):
                    arrived(there, self.part(s, "side"), self.side_sem.at[s])
                    self.go(both(there, on), s, "side", to)

        def ready(self, h):
            found = []
            for level, there in (
                ((z, None),) if h == 0 else ((z - h, z - h >= 0), (z + h, z + h < levels))
            ):
                found.append((there, level * cols + x, None))
                for s in self.peers(level):
                    found.append(
                        (
                            there,
                            s,
                            functools.partial(
                                arrived, None, self.part(s, "main"), self.main_sem.at[s]
                            ),
                        )
                    )
            return found

    spread_in = Spread(wi, sem_in, sem_in_side)
    spread_out = Spread(wo, sem_out, sem_out_side)
    for copy in locals_[:n_in]:
        copy.wait()
    spread_in.begin()

    mine = pl.ds(pl.multiple_of(t * rows, rows), rows)
    wide = tok[...].astype(F32)
    inverse = lax.rsqrt(jnp.mean(wide * wide, axis=1, keepdims=True) + EPS)
    for i in range(n_sp):
        span = slice(i * piece, (i + 1) * piece)
        xs[i, mine, :] = (tok[:, span].astype(F32) * inverse * gain[:, span]).astype(BF16)

    def rows_of(device):
        return xs.at[:, pl.ds(pl.multiple_of(device * rows, rows), rows), :]

    for d in range(1, chips):
        send(None, rows_of(t), rows_of(t), sem_tok.at[t], (me, (y + d) % chips * CORES + c))
    send(None, rows_of(t), rows_of(t), sem_tok.at[t], (me, partner))

    spread_in.begin_side()
    for h in range(1, levels - 1):
        spread_in.hop(h)
    for copy in locals_[n_in:]:
        copy.wait()

    for d in range(1, chips):
        far = (y + chips - d) % chips * CORES + c
        arrived(None, rows_of(far), sem_tok.at[far])
        send(None, rows_of(far), rows_of(far), sem_tok.at[far], (me, partner))
    arrived(None, rows_of(partner), sem_tok.at[partner])
    for d in range(1, chips):
        far = (y + chips - d) % chips * CORES + (1 - c)
        arrived(None, rows_of(far), sem_tok.at[far])

    tile = row_tile(seq, 256)

    def project(s, first):
        @pl.loop(0, seq // tile)
        def _(i):
            r = pl.ds(pl.multiple_of(i * tile, tile), tile)
            value = jnp.dot(xs[s, r, :], wi[s], preferred_element_type=F32)
            if first:
                acc[r, :] = value
            else:
                acc[r, :] += value

    def project_ready(h):
        for i, (cond, s, wait) in enumerate(spread_in.ready(h)):

            def run(s=s, wait=wait, first=(h == 0 and i == 0)):
                if wait is not None:
                    wait()
                project(s, first)

            when(cond, run)

    for h in range(levels - 1):
        project_ready(h)
    spread_in.hop(levels - 1)
    spread_out.begin()
    project_ready(levels - 1)

    @pl.loop(0, seq // tile)
    def _(i):
        i = seq // tile - 1 - i
        r = pl.multiple_of(i * tile, tile)
        ext[pl.ds(pl.multiple_of(r + WINDOW, WINDOW), tile), :] = acc[pl.ds(r, tile), :].astype(BF16)

    halo = kw + vw + pw
    later, earlier = me + 1 < n_sp, me > 0
    head = ext.at[pl.ds(0, WINDOW), pl.ds(qw, halo)]
    send(later, ext.at[pl.ds(seq, WINDOW), pl.ds(qw, halo)], head, sem_halo.at[0], (me + 1, t))

    channel0 = qw + kw + vw
    group = t * pw // POOL_CH
    whole_prefix = group == POOL_GROUPS - 1
    total = jnp.sum(ext[WINDOW:, channel0:].astype(F32), axis=0, keepdims=True)
    tot[me] = jnp.broadcast_to(total, tot.shape[1:])
    for d in range(1, n_sp):
        send(
            both(whole_prefix, me + d < n_sp), tot.at[me], tot.at[me], sem_tot.at[me],
            (me + d, t),
        )

    group_heads = qw // kw
    stacked = group_heads * WINDOW
    scale = HEAD_DIM ** (-0.5)

    def attend(n):
        q_rows = pl.ds(pl.multiple_of(n * WINDOW + WINDOW, WINDOW), WINDOW)
        k_rows = pl.ds(pl.multiple_of(n * WINDOW, WINDOW), 2 * WINDOW)
        queries = ext[q_rows, :qw]
        keys = ext[k_rows, qw : qw + kw]
        values = ext[k_rows, qw + kw : channel0]
        row = lax.broadcasted_iota(jnp.int32, (stacked, 2 * WINDOW), 0)
        q_index = row % WINDOW
        k_index = lax.broadcasted_iota(jnp.int32, (stacked, 2 * WINDOW), 1)
        lowest = jnp.where(me * blocks + n == 0, WINDOW, 0)
        allowed = (k_index > q_index) & (k_index <= q_index + WINDOW) & (k_index >= lowest)
        which = lax.broadcasted_iota(jnp.int32, (stacked, 1), 0) // WINDOW
        done = []
        for j in range(kw // HEAD_DIM):
            part = slice(j * HEAD_DIM, (j + 1) * HEAD_DIM)
            first = j * group_heads
            q = jnp.concatenate(
                [
                    queries[:, (first + g) * HEAD_DIM : (first + g + 1) * HEAD_DIM]
                    for g in range(group_heads)
                ],
                axis=0,
            )
            scores = (
                lax.dot_general(
                    q, keys[:, part], (((1,), (1,)), ((), ())), preferred_element_type=F32
                )
                * scale
            )
            scores = jnp.where(allowed, scores, -jnp.inf)
            sinks = jnp.full((stacked, 1), sink[first], F32)
            for g in range(1, group_heads):
                sinks = jnp.where(which == g, sink[first + g], sinks)
            peak = jnp.maximum(jnp.max(scores, axis=1, keepdims=True), sinks)
            expo = jnp.exp(scores - peak)
            denom = jnp.sum(expo, axis=1, keepdims=True) + jnp.exp(sinks - peak)
            probs = (expo * (1.0 / denom)).astype(BF16)
            got = jnp.dot(probs, values[:, part], preferred_element_type=F32)
            done += [got[g * WINDOW : (g + 1) * WINDOW] for g in range(group_heads)]
        to = pl.ds(pl.multiple_of(n * WINDOW, WINDOW), WINDOW)
        mix[to, :qw] = jnp.concatenate(done, axis=1).astype(BF16)

    inner = blocks - 1
    stages = max(1, levels - 1)
    cuts = [1 + inner * i // stages for i in range(stages + 1)]
    for i in range(stages):
        pl.loop(cuts[i], cuts[i + 1])(attend)
        if i == 0:
            spread_out.begin_side()
        if i + 1 < levels - 1:
            spread_out.hop(i + 1)

    @pl.when(jnp.logical_not(earlier))
    def _():
        ext[:WINDOW, qw:] = jnp.zeros((WINDOW, halo), BF16)

    arrived(earlier, head, sem_halo.at[0])
    attend(0)

    carry[...] = jnp.zeros(carry.shape, F32)
    for d in range(1, n_sp):

        def add(d=d):
            arrived(None, tot.at[me - d], sem_tot.at[me - d])
            carry[...] += tot[me - d]

        when(both(whole_prefix, me - d >= 0), add)

    reach = jnp.where(
        group == 0, SHORT_REACHES[0], jnp.where(group == 1, SHORT_REACHES[1], WINDOW)
    )
    reach = jnp.where(whole_prefix, n_sp * seq, reach)
    lowest = jnp.where(whole_prefix, WINDOW, 0)

    @pl.loop(0, blocks)
    def _(n):
        q_index = lax.broadcasted_iota(jnp.int32, (WINDOW, 2 * WINDOW), 0)
        k_index = lax.broadcasted_iota(jnp.int32, (WINDOW, 2 * WINDOW), 1)
        distance = q_index + WINDOW - k_index
        band = (distance >= 0) & (distance < reach) & (k_index >= lowest)
        band = jnp.where(band, 1.0, 0.0).astype(BF16)
        k_rows = pl.ds(pl.multiple_of(n * WINDOW, WINDOW), 2 * WINDOW)
        both_blocks = ext[k_rows, channel0:]
        sums = jnp.dot(band, both_blocks, preferred_element_type=F32) + carry[0:1, :]
        position = me * seq + n * WINDOW + lax.broadcasted_iota(jnp.int32, (WINDOW, 1), 0)
        counted = jnp.minimum(position + 1, reach).astype(F32)
        mixed = (sums / counted - both_blocks[WINDOW:].astype(F32)) * pgain[...]
        mix[pl.ds(pl.multiple_of(n * WINDOW, WINDOW), WINDOW), qw:] = mixed.astype(BF16)
        carry[...] = jnp.where(
            whole_prefix, jnp.broadcast_to(sums[WINDOW - 1 :], carry.shape), 0.0
        )

    def mix_rows(chip, core):
        return mix[pl.ds(pl.multiple_of((chip * CORES + core) * rows, rows), rows), :]

    outs = []

    def multiply(cond, s, wait):
        def run():
            if wait is not None:
                wait()
            for chip in range(chips):
                dsend[s, chip] = jnp.dot(
                    mix_rows(chip, 1 - c), wo[s], preferred_element_type=F32
                ).astype(BF16)

        when(cond, run)
        send(cond, dsend.at[s], drecv.at[s], sem_core.at[s], (me, partner))

        def keep():
            for chip in range(chips):
                own[s, chip] = jnp.dot(mix_rows(chip, c), wo[s], preferred_element_type=F32)

        when(cond, keep)

    def finish(cond, s):
        arrived(cond, drecv.at[s], sem_core.at[s])
        for d in range(1, chips):
            far = (y + d) % chips

            def pack(d=d, far=far):
                ysend[s, d - 1] = (own[s, far] + drecv[s, far].astype(F32)).astype(BF16)

            when(cond, pack)
            send(
                cond, ysend.at[s, d - 1], yrecv.at[s, d - 1], sem_y.at[s, d - 1],
                (me, far * CORES + c),
            )

    pending = None
    for h in range(levels):
        if h == levels - 1:
            if pending is not None:
                finish(*pending)
                pending = None
            spread_out.hop(h)
        for cond, s, wait in spread_out.ready(h):
            multiply(cond, s, wait)
            if pending is not None:
                finish(*pending)
            pending = (cond, s)
    finish(*pending)

    for i in range(n_sp):
        value = own[i, y] + drecv[i, y].astype(F32)
        for d in range(1, chips):
            arrived(None, yrecv.at[i, d - 1], sem_y.at[i, d - 1])
            value += yrecv[i, d - 1].astype(F32)
        w = wo.shape[2]
        out[:, i * w : (i + 1) * w] = value.astype(BF16)

    for cond, copy in sent:
        when(cond, copy.wait_send)


def local(
    n_sp, n_tp, tokens_in, norm_gain, query_weight, key_weight, value_weight, pool_weight,
    sink_logit, pool_gain, attention_out_weight, pool_out_weight,
):
    rows, depth = tokens_in.shape
    seq = rows * n_tp
    ins = [query_weight, key_weight, value_weight, pool_weight]
    outs = [attention_out_weight, pool_out_weight]
    widths = tuple(w.shape[1] for w in ins)
    if any(w % 128 for w in widths):
        ins = [jnp.concatenate(ins, axis=1)]
    cols = math.gcd(n_sp, max(1, n_tp // CORES))
    levels, chips = n_sp // cols, n_tp // CORES
    k_in, k_out = ins[0].shape[0], sum(w.shape[0] for w in outs)
    width, out_cols = sum(widths), outs[0].shape[1]
    pw = widths[3]
    hops = 2 * (levels - 1) + 1
    n_send = 2 * (2 + 2 * cols + hops * (2 + 3 * cols)) + 2 * n_tp + n_sp + 2
    n_send += 2 * n_sp * hops * chips
    vmem = pl.BlockSpec(memory_space=pltpu.VMEM)
    hbm = pl.BlockSpec(memory_space=pl.ANY)
    dma = pltpu.SemaphoreType.DMA
    return pl.pallas_call(
        functools.partial(kernel, n_sp, n_tp, cols, len(ins), len(outs), widths),
        out_shape=jax.ShapeDtypeStruct((rows, depth), BF16),
        in_specs=[vmem, vmem, pl.BlockSpec(memory_space=pltpu.SMEM), vmem]
        + [hbm] * (len(ins) + len(outs)),
        out_specs=vmem,
        scratch_shapes=[
            pltpu.VMEM((n_sp, seq, depth // n_sp), BF16),
            pltpu.VMEM((n_sp, k_in, width), BF16),
            pltpu.VMEM((n_sp, k_out, out_cols), BF16),
            pltpu.VMEM((seq, width), F32),
            pltpu.VMEM((seq + WINDOW, width), BF16),
            pltpu.VMEM((seq, widths[0] + pw), BF16),
            pltpu.VMEM((n_sp, 8, pw), F32),
            pltpu.VMEM((8, pw), F32),
            pltpu.VMEM((n_sp, chips, rows, out_cols), BF16),
            pltpu.VMEM((n_sp, chips, rows, out_cols), BF16),
            pltpu.VMEM((n_sp, max(1, chips - 1), rows, out_cols), BF16),
            pltpu.VMEM((n_sp, max(1, chips - 1), rows, out_cols), BF16),
            pltpu.VMEM((n_sp, chips, rows, out_cols), F32),
            dma((len(ins) + len(outs),)),
            dma((n_send,)),
            dma((n_sp,)),
            dma((n_sp,)),
            dma((n_sp,)),
            dma((n_sp,)),
            dma((n_tp,)),
            dma((1,)),
            dma((n_sp,)),
            dma((n_sp,)),
            dma((n_sp, max(1, chips - 1))),
        ],
        compiler_params=pltpu.CompilerParams(
            collective_id=0, has_side_effects=True, vmem_limit_bytes=58 << 20
        ),
    )(
        tokens_in, norm_gain.reshape(1, -1), sink_logit, pool_gain.reshape(1, -1), *ins, *outs
    )


def solution(mesh):
    in_specs = (
        P(("sp", "tp"), None), P(), P("sp", "tp"), P("sp", "tp"), P("sp", "tp"), P("sp", "tp"),
        P("tp"), P("tp"), P("tp", "sp"), P("tp", "sp"),
    )
    out_specs = P(("sp", "tp"), None)
    return jax.shard_map(
        functools.partial(local, mesh.shape["sp"], mesh.shape["tp"]),
        mesh=mesh, in_specs=in_specs, out_specs=out_specs, check_vma=False,
    )
```

```python
import functools
import math

import jax
import jax.numpy as jnp
from jax import lax
from jax.experimental import pallas as pl
from jax.experimental.pallas import tpu as pltpu
from jax.sharding import PartitionSpec as P

HEAD_DIM = 64
POOL_CH = 256
POOL_GROUPS = 4
WINDOW = 128
EPS = 1e-06
SHORT_REACHES = (8, 32)
CORES = 2
SIDE_SHARE = 0.4
MESH = pl.DeviceIdType.MESH
F32 = jnp.float32
BF16 = jnp.bfloat16


def row_tile(rows, most):
    tile = most
    while rows % tile:
        tile -= 16
    return tile


def kernel(n_sp, n_tp, cols, n_in, n_out, widths, *refs):
    tok, gain, sink, pgain = refs[:4]
    win_refs = refs[4 : 4 + n_in]
    wout_refs = refs[4 + n_in : 4 + n_in + n_out]
    (
        out, tokv, xs, wq, wp, wo, accq, accp, ext, mix, tot, carry, dsend, drecv, ysend, yrecv, own,
        local_sem, send_sem, sem_q, sem_p, sem_out, sem_out_side,
        sem_tok, sem_halo, sem_tot, sem_core, sem_y,
    ) = refs[4 + n_in + n_out :]
    qw, kw, vw, pw = widths
    levels = n_sp // cols
    chips = n_tp // CORES
    rows, seq = tok.shape[0], xs.shape[1]
    qkv = wq.shape[2]
    piece = xs.shape[2]
    blocks = seq // WINDOW
    me, t = lax.axis_index("sp"), lax.axis_index("tp")
    z, x = me // cols, me % cols
    y, c = t // CORES, t % CORES
    partner = y * CORES + (1 - c)

    locals_ = []
    at = 0
    for i, ref in enumerate(win_refs[:-1]):
        w = ref.shape[1]
        locals_.append(pltpu.make_async_copy(ref, wq.at[me, :, pl.ds(at, w)], local_sem.at[i]))
        at += w
    locals_.append(pltpu.make_async_copy(win_refs[-1], wp.at[me], local_sem.at[n_in - 1]))
    at = 0
    for i, ref in enumerate(wout_refs):
        k = ref.shape[0]
        locals_.append(
            pltpu.make_async_copy(ref, wo.at[me, pl.ds(at, k), :], local_sem.at[n_in + i])
        )
        at += k
    tok_copy = pltpu.make_async_copy(tok, tokv, local_sem.at[n_in + n_out])
    for copy in locals_[:n_in] + [tok_copy] + locals_[n_in:]:
        copy.start()

    barrier = pltpu.get_barrier_semaphore()
    for d in range(1, n_sp):
        pl.semaphore_signal(barrier, inc=1, device_id=((me + d) % n_sp, t), device_id_type=MESH)
    for d in range(1, n_tp):
        pl.semaphore_signal(barrier, inc=1, device_id=(me, (t + d) % n_tp), device_id_type=MESH)
    pl.semaphore_wait(barrier, n_sp + n_tp - 2)

    sent = []

    def when(cond, fn):
        if cond is None:
            fn()
        else:
            pl.when(cond)(fn)

    def both(a, b):
        return b if a is None else (a if b is None else jnp.logical_and(a, b))

    def send(cond, src, dst, recv, dev):
        copy = pltpu.make_async_remote_copy(
            src_ref=src, dst_ref=dst, send_sem=send_sem.at[len(sent)], recv_sem=recv,
            device_id=dev, device_id_type=MESH,
        )
        when(cond, copy.start)
        sent.append((cond, copy))

    def arrived(cond, dst, recv):
        copy = pltpu.make_async_remote_copy(
            src_ref=dst, dst_ref=dst, send_sem=send_sem.at[0], recv_sem=recv,
            device_id=(me, partner), device_id_type=MESH,
        )
        when(cond, copy.wait_recv)

    up, down = z + 1 < levels, z > 0

    class Spread:
        def __init__(self, buf, main_sem, side_sem):
            self.buf, self.main_sem, self.side_sem = buf, main_sem, side_sem
            k = buf.shape[1]
            self.side = 0 if side_sem is None else max(16, int(k * SIDE_SHARE) // 16 * 16)
            self.main = k - self.side

        def part(self, s, which):
            if which == "all":
                return self.buf.at[s]
            if which == "main":
                return self.buf.at[s, pl.ds(0, self.main), :]
            return self.buf.at[s, pl.ds(self.main, self.side), :]

        def go(self, cond, s, which, dev_sp):
            if which == "side" and not self.side:
                return
            sem = self.side_sem if which == "side" else self.main_sem
            ref = self.part(s, which)
            send(cond, ref, ref, sem.at[s], (dev_sp, t))

        def across(self, cond, s, which):
            for d in range(1, cols):
                self.go(cond, s, which, z * cols + (x + d) % cols)

        def peers(self, level):
            return [level * cols + (x + cols - d) % cols for d in range(1, cols)]

        def begin(self):
            self.across(None, me, "side")
            self.go(up, me, "all", me + cols)
            self.go(down, me, "all", me - cols)
            self.across(None, me, "main")

        def begin_side(self):
            for s in self.peers(z) if self.side else []:
                arrived(None, self.part(s, "side"), self.side_sem.at[s])
                self.go(up, s, "side", me + cols)
                self.go(down, s, "side", me - cols)

        def hop(self, h):
            for level, there, on, to in (
                (z - h, z - h >= 0, up, me + cols),
                (z + h, z + h < levels, down, me - cols),
            ):
                s = level * cols + x
                arrived(there, self.part(s, "all"), self.main_sem.at[s])
                self.go(both(there, on), s, "all", to)
                self.across(there, s, "main")
                for s in self.peers(level) if self.side else []:
                    arrived(there, self.part(s, "side"), self.side_sem.at[s])
                    self.go(both(there, on), s, "side", to)

        def ready(self, h):
            found = []
            for level, there in (
                ((z, None),) if h == 0 else ((z - h, z - h >= 0), (z + h, z + h < levels))
            ):
                found.append((there, level * cols + x, None))
                for s in self.peers(level):
                    found.append(
                        (
                            there,
                            s,
                            functools.partial(
                                arrived, None, self.part(s, "main"), self.main_sem.at[s]
                            ),
                        )
                    )
            return found

    spread_q = Spread(wq, sem_q, None)
    spread_p = Spread(wp, sem_p, None)
    spread_out = Spread(wo, sem_out, sem_out_side)
    for copy in locals_[:n_in]:
        copy.wait()
    spread_q.begin()
    spread_p.begin()
    tok_copy.wait()

    mine = pl.ds(pl.multiple_of(t * rows, rows), rows)
    wide = tokv[...].astype(F32)
    inverse = lax.rsqrt(jnp.mean(wide * wide, axis=1, keepdims=True) + EPS)
    for i in range(n_sp):
        span = slice(i * piece, (i + 1) * piece)
        xs[i, mine, :] = (tokv[:, span].astype(F32) * inverse * gain[:, span]).astype(BF16)

    def rows_of(device):
        return xs.at[:, pl.ds(pl.multiple_of(device * rows, rows), rows), :]

    for d in range(1, chips):
        send(None, rows_of(t), rows_of(t), sem_tok.at[t], (me, (y + d) % chips * CORES + c))
    send(None, rows_of(t), rows_of(t), sem_tok.at[t], (me, partner))

    for h in range(1, levels - 1):
        spread_q.hop(h)
        if h < levels - 2:
            spread_p.hop(h)

    for d in range(1, chips):
        far = (y + chips - d) % chips * CORES + c
        arrived(None, rows_of(far), sem_tok.at[far])
        send(None, rows_of(far), rows_of(far), sem_tok.at[far], (me, partner))
    arrived(None, rows_of(partner), sem_tok.at[partner])
    for d in range(1, chips):
        far = (y + chips - d) % chips * CORES + (1 - c)
        arrived(None, rows_of(far), sem_tok.at[far])

    spread_q.hop(levels - 1)
    for h in range(max(1, levels - 2), levels - 1):
        spread_p.hop(h)

    tile = row_tile(seq, 256)

    def project(spread, acc, h):
        for i, (cond, s, wait) in enumerate(spread.ready(h)):

            def run(s=s, wait=wait, first=(h == 0 and i == 0)):
                if wait is not None:
                    wait()

                @pl.loop(0, seq // tile)
                def _(i):
                    r = pl.ds(pl.multiple_of(i * tile, tile), tile)
                    value = jnp.dot(xs[s, r, :], spread.buf[s], preferred_element_type=F32)
                    if first:
                        acc[r, :] = value
                    else:
                        acc[r, :] += value

            when(cond, run)

    def settle(acc, at):
        @pl.loop(0, seq // tile)
        def _(i):
            r = pl.multiple_of(i * tile, tile)
            to = pl.ds(pl.multiple_of(r + WINDOW, WINDOW), tile)
            ext[to, at : at + acc.shape[1]] = acc[pl.ds(r, tile), :].astype(BF16)

    later, earlier = me + 1 < n_sp, me > 0

    def pass_on(at, width, i):
        head = ext.at[pl.ds(0, WINDOW), pl.ds(at, width)]
        tail = ext.at[pl.ds(seq, WINDOW), pl.ds(at, width)]
        send(later, tail, head, sem_halo.at[i], (me + 1, t))
        return head

    for h in range(levels - 1):
        project(spread_q, accq, h)
    spread_p.hop(levels - 1)
    for copy in locals_[n_in:]:
        copy.wait()
    spread_out.begin()
    project(spread_q, accq, levels - 1)
    settle(accq, 0)
    head_kv = pass_on(qw, kw + vw, 0)
    channel0 = qkv
    group = t * pw // POOL_CH
    whole_prefix = group == POOL_GROUPS - 1

    group_heads = qw // kw
    stacked = group_heads * WINDOW
    scale = HEAD_DIM ** (-0.5)

    def attend(n):
        q_rows = pl.ds(pl.multiple_of(n * WINDOW + WINDOW, WINDOW), WINDOW)
        k_rows = pl.ds(pl.multiple_of(n * WINDOW, WINDOW), 2 * WINDOW)
        queries = ext[q_rows, :qw]
        keys = ext[k_rows, qw : qw + kw]
        values = ext[k_rows, qw + kw : channel0]
        row = lax.broadcasted_iota(jnp.int32, (stacked, 2 * WINDOW), 0)
        q_index = row % WINDOW
        k_index = lax.broadcasted_iota(jnp.int32, (stacked, 2 * WINDOW), 1)
        lowest = jnp.where(me * blocks + n == 0, WINDOW, 0)
        allowed = (k_index > q_index) & (k_index <= q_index + WINDOW) & (k_index >= lowest)
        which = lax.broadcasted_iota(jnp.int32, (stacked, 1), 0) // WINDOW
        done = []
        for j in range(kw // HEAD_DIM):
            part = slice(j * HEAD_DIM, (j + 1) * HEAD_DIM)
            first = j * group_heads
            q = jnp.concatenate(
                [
                    queries[:, (first + g) * HEAD_DIM : (first + g + 1) * HEAD_DIM]
                    for g in range(group_heads)
                ],
                axis=0,
            )
            scores = (
                lax.dot_general(
                    q, keys[:, part], (((1,), (1,)), ((), ())), preferred_element_type=F32
                )
                * scale
            )
            scores = jnp.where(allowed, scores, -jnp.inf)
            sinks = jnp.full((stacked, 1), sink[first], F32)
            for g in range(1, group_heads):
                sinks = jnp.where(which == g, sink[first + g], sinks)
            peak = jnp.maximum(jnp.max(scores, axis=1, keepdims=True), sinks)
            expo = jnp.exp(scores - peak)
            denom = jnp.sum(expo, axis=1, keepdims=True) + jnp.exp(sinks - peak)
            probs = (expo * (1.0 / denom)).astype(BF16)
            got = jnp.dot(probs, values[:, part], preferred_element_type=F32)
            done += [got[g * WINDOW : (g + 1) * WINDOW] for g in range(group_heads)]
        to = pl.ds(pl.multiple_of(n * WINDOW, WINDOW), WINDOW)
        mix[to, :qw] = jnp.concatenate(done, axis=1).astype(BF16)

    spread_out.begin_side()
    spread_out.hop(1)
    third = max(2, (blocks + 1) // 2)
    pl.loop(1, third)(attend)
    spread_out.hop(2)
    for h in range(levels):
        project(spread_p, accp, h)
    settle(accp, channel0)
    head_pool = pass_on(channel0, pw, 1)
    total = jnp.sum(ext[WINDOW:, channel0:].astype(F32), axis=0, keepdims=True)
    tot[me] = jnp.broadcast_to(total, tot.shape[1:])
    for d in range(1, n_sp):
        send(
            both(whole_prefix, me + d < n_sp), tot.at[me], tot.at[me], sem_tot.at[me],
            (me + d, t),
        )
    pl.loop(third, blocks)(attend)

    @pl.when(jnp.logical_not(earlier))
    def _():
        ext[:WINDOW, qw:] = jnp.zeros((WINDOW, ext.shape[1] - qw), BF16)

    arrived(earlier, head_kv, sem_halo.at[0])
    attend(0)
    arrived(earlier, head_pool, sem_halo.at[1])

    carry[...] = jnp.zeros(carry.shape, F32)
    for d in range(1, n_sp):

        def add(d=d):
            arrived(None, tot.at[me - d], sem_tot.at[me - d])
            carry[...] += tot[me - d]

        when(both(whole_prefix, me - d >= 0), add)

    reach = jnp.where(
        group == 0, SHORT_REACHES[0], jnp.where(group == 1, SHORT_REACHES[1], WINDOW)
    )
    reach = jnp.where(whole_prefix, n_sp * seq, reach)
    lowest = jnp.where(whole_prefix, WINDOW, 0)

    @pl.loop(0, blocks)
    def _(n):
        q_index = lax.broadcasted_iota(jnp.int32, (WINDOW, 2 * WINDOW), 0)
        k_index = lax.broadcasted_iota(jnp.int32, (WINDOW, 2 * WINDOW), 1)
        distance = q_index + WINDOW - k_index
        band = (distance >= 0) & (distance < reach) & (k_index >= lowest)
        band = jnp.where(band, 1.0, 0.0).astype(BF16)
        k_rows = pl.ds(pl.multiple_of(n * WINDOW, WINDOW), 2 * WINDOW)
        both_blocks = ext[k_rows, channel0:]
        sums = jnp.dot(band, both_blocks, preferred_element_type=F32) + carry[0:1, :]
        position = me * seq + n * WINDOW + lax.broadcasted_iota(jnp.int32, (WINDOW, 1), 0)
        counted = jnp.minimum(position + 1, reach).astype(F32)
        mixed = (sums / counted - both_blocks[WINDOW:].astype(F32)) * pgain[...]
        mix[pl.ds(pl.multiple_of(n * WINDOW, WINDOW), WINDOW), qw:] = mixed.astype(BF16)
        carry[...] = jnp.where(
            whole_prefix, jnp.broadcast_to(sums[WINDOW - 1 :], carry.shape), 0.0
        )

    def mix_rows(chip, core):
        return mix[pl.ds(pl.multiple_of((chip * CORES + core) * rows, rows), rows), :]

    outs = []

    def multiply(cond, s, wait):
        def run():
            if wait is not None:
                wait()
            for chip in range(chips):
                dsend[s, chip] = jnp.dot(
                    mix_rows(chip, 1 - c), wo[s], preferred_element_type=F32
                ).astype(BF16)

        when(cond, run)
        send(cond, dsend.at[s], drecv.at[s], sem_core.at[s], (me, partner))

        def keep():
            for chip in range(chips):
                own[s, chip] = jnp.dot(mix_rows(chip, c), wo[s], preferred_element_type=F32)

        when(cond, keep)

    def finish(cond, s):
        arrived(cond, drecv.at[s], sem_core.at[s])
        for d in range(1, chips):
            far = (y + d) % chips

            def pack(d=d, far=far):
                ysend[s, d - 1] = (own[s, far] + drecv[s, far].astype(F32)).astype(BF16)

            when(cond, pack)
            send(
                cond, ysend.at[s, d - 1], yrecv.at[s, d - 1], sem_y.at[s, d - 1],
                (me, far * CORES + c),
            )

    pending = None
    for h in range(levels):
        if h == levels - 1:
            if pending is not None:
                finish(*pending)
                pending = None
            spread_out.hop(h)
        for cond, s, wait in spread_out.ready(h):
            multiply(cond, s, wait)
            if pending is not None:
                finish(*pending)
            pending = (cond, s)
    finish(*pending)

    for i in range(n_sp):
        value = own[i, y] + drecv[i, y].astype(F32)
        for d in range(1, chips):
            arrived(None, yrecv.at[i, d - 1], sem_y.at[i, d - 1])
            value += yrecv[i, d - 1].astype(F32)
        w = wo.shape[2]
        out[:, i * w : (i + 1) * w] = value.astype(BF16)

    for cond, copy in sent:
        when(cond, copy.wait_send)


def local(
    n_sp, n_tp, tokens_in, norm_gain, query_weight, key_weight, value_weight, pool_weight,
    sink_logit, pool_gain, attention_out_weight, pool_out_weight,
):
    rows, depth = tokens_in.shape
    seq = rows * n_tp
    ins = [query_weight, key_weight, value_weight, pool_weight]
    outs = [attention_out_weight, pool_out_weight]
    widths = tuple(w.shape[1] for w in ins)
    if any(w % 128 for w in widths):
        ins = [jnp.concatenate(ins[:3], axis=1), ins[3]]
    cols = math.gcd(n_sp, max(1, n_tp // CORES))
    levels, chips = n_sp // cols, n_tp // CORES
    k_in, k_out = ins[0].shape[0], sum(w.shape[0] for w in outs)
    width, out_cols = sum(widths), outs[0].shape[1]
    pw = widths[3]
    hops = 2 * (levels - 1) + 1
    n_send = 3 * (2 + 2 * cols + hops * (2 + 3 * cols)) + 2 * n_tp + n_sp + 2
    n_send += 2 * n_sp * hops * chips
    vmem = pl.BlockSpec(memory_space=pltpu.VMEM)
    hbm = pl.BlockSpec(memory_space=pl.ANY)
    dma = pltpu.SemaphoreType.DMA
    return pl.pallas_call(
        functools.partial(kernel, n_sp, n_tp, cols, len(ins), len(outs), widths),
        out_shape=jax.ShapeDtypeStruct((rows, depth), BF16),
        in_specs=[hbm, vmem, pl.BlockSpec(memory_space=pltpu.SMEM), vmem]
        + [hbm] * (len(ins) + len(outs)),
        out_specs=vmem,
        scratch_shapes=[
            pltpu.VMEM((rows, depth), BF16),
            pltpu.VMEM((n_sp, seq, depth // n_sp), BF16),
            pltpu.VMEM((n_sp, k_in, width - pw), BF16),
            pltpu.VMEM((n_sp, k_in, pw), BF16),
            pltpu.VMEM((n_sp, k_out, out_cols), BF16),
            pltpu.VMEM((seq, width - pw), F32),
            pltpu.VMEM((seq, pw), F32),
            pltpu.VMEM((seq + WINDOW, width), BF16),
            pltpu.VMEM((seq, widths[0] + pw), BF16),
            pltpu.VMEM((n_sp, 8, pw), F32),
            pltpu.VMEM((8, pw), F32),
            pltpu.VMEM((n_sp, chips, rows, out_cols), BF16),
            pltpu.VMEM((n_sp, chips, rows, out_cols), BF16),
            pltpu.VMEM((n_sp, max(1, chips - 1), rows, out_cols), BF16),
            pltpu.VMEM((n_sp, max(1, chips - 1), rows, out_cols), BF16),
            pltpu.VMEM((n_sp, chips, rows, out_cols), F32),
            dma((len(ins) + len(outs) + 1,)),
            dma((n_send,)),
            dma((n_sp,)),
            dma((n_sp,)),
            dma((n_sp,)),
            dma((n_sp,)),
            dma((n_tp,)),
            dma((2,)),
            dma((n_sp,)),
            dma((n_sp,)),
            dma((n_sp, max(1, chips - 1))),
        ],
        compiler_params=pltpu.CompilerParams(
            collective_id=0, has_side_effects=True, vmem_limit_bytes=58 << 20
        ),
    )(
        tokens_in, norm_gain.reshape(1, -1), sink_logit, pool_gain.reshape(1, -1), *ins, *outs
    )


def solution(mesh):
    in_specs = (
        P(("sp", "tp"), None), P(), P("sp", "tp"), P("sp", "tp"), P("sp", "tp"), P("sp", "tp"),
        P("tp"), P("tp"), P("tp", "sp"), P("tp", "sp"),
    )
    out_specs = P(("sp", "tp"), None)
    return jax.shard_map(
        functools.partial(local, mesh.shape["sp"], mesh.shape["tp"]),
        mesh=mesh, in_specs=in_specs, out_specs=out_specs, check_vma=False,
    )
```

```python
import functools
import math

import jax
import jax.numpy as jnp
from jax import lax
from jax.experimental import pallas as pl
from jax.experimental.pallas import tpu as pltpu
from jax.sharding import PartitionSpec as P

HEAD_DIM = 64
POOL_CH = 256
POOL_GROUPS = 4
WINDOW = 128
EPS = 1e-06
SHORT_REACHES = (8, 32)
CORES = 2
SIDE_SHARE = 0.3
MESH = pl.DeviceIdType.MESH
F32 = jnp.float32
BF16 = jnp.bfloat16


def row_tile(rows, most):
    tile = most
    while rows % tile:
        tile -= 16
    return tile


def kernel(n_sp, n_tp, cols, n_in, n_out, widths, *refs):
    tok, gain, sink, pgain = refs[:4]
    win_refs = refs[4 : 4 + n_in]
    wout_refs = refs[4 + n_in : 4 + n_in + n_out]
    (
        out, tokv, xs, wq, wp, wo, accq, accp, ext, mix, tot, carry, dsend, drecv, ysend, yrecv, own,
        local_sem, send_sem, sem_q, sem_p, sem_p_side, sem_out, sem_out_side,
        sem_tok, sem_halo, sem_tot, sem_core, sem_y,
    ) = refs[4 + n_in + n_out :]
    qw, kw, vw, pw = widths
    levels = n_sp // cols
    chips = n_tp // CORES
    rows, seq = tok.shape[0], xs.shape[1]
    qkv = wq.shape[2]
    piece = xs.shape[2]
    blocks = seq // WINDOW
    me, t = lax.axis_index("sp"), lax.axis_index("tp")
    z, x = me // cols, me % cols
    y, c = t // CORES, t % CORES
    partner = y * CORES + (1 - c)

    locals_ = []
    at = 0
    for i, ref in enumerate(win_refs[:-1]):
        w = ref.shape[1]
        locals_.append(pltpu.make_async_copy(ref, wq.at[me, :, pl.ds(at, w)], local_sem.at[i]))
        at += w
    locals_.append(pltpu.make_async_copy(win_refs[-1], wp.at[me], local_sem.at[n_in - 1]))
    at = 0
    for i, ref in enumerate(wout_refs):
        k = ref.shape[0]
        locals_.append(
            pltpu.make_async_copy(ref, wo.at[me, pl.ds(at, k), :], local_sem.at[n_in + i])
        )
        at += k
    tok_copy = pltpu.make_async_copy(tok, tokv, local_sem.at[n_in + n_out])
    for copy in locals_[:n_in] + [tok_copy] + locals_[n_in:]:
        copy.start()

    barrier = pltpu.get_barrier_semaphore()
    for d in range(1, n_sp):
        pl.semaphore_signal(barrier, inc=1, device_id=((me + d) % n_sp, t), device_id_type=MESH)
    for d in range(1, n_tp):
        pl.semaphore_signal(barrier, inc=1, device_id=(me, (t + d) % n_tp), device_id_type=MESH)
    pl.semaphore_wait(barrier, n_sp + n_tp - 2)

    sent = []

    def when(cond, fn):
        if cond is None:
            fn()
        else:
            pl.when(cond)(fn)

    def both(a, b):
        return b if a is None else (a if b is None else jnp.logical_and(a, b))

    def send(cond, src, dst, recv, dev):
        copy = pltpu.make_async_remote_copy(
            src_ref=src, dst_ref=dst, send_sem=send_sem.at[len(sent)], recv_sem=recv,
            device_id=dev, device_id_type=MESH,
        )
        when(cond, copy.start)
        sent.append((cond, copy))

    def arrived(cond, dst, recv):
        copy = pltpu.make_async_remote_copy(
            src_ref=dst, dst_ref=dst, send_sem=send_sem.at[0], recv_sem=recv,
            device_id=(me, partner), device_id_type=MESH,
        )
        when(cond, copy.wait_recv)

    up, down = z + 1 < levels, z > 0

    class Spread:
        def __init__(self, buf, main_sem, side_sem):
            self.buf, self.main_sem, self.side_sem = buf, main_sem, side_sem
            k = buf.shape[1]
            self.side = 0 if side_sem is None else max(16, int(k * SIDE_SHARE) // 16 * 16)
            self.main = k - self.side

        def part(self, s, which):
            if which == "all":
                return self.buf.at[s]
            if which == "main":
                return self.buf.at[s, pl.ds(0, self.main), :]
            return self.buf.at[s, pl.ds(self.main, self.side), :]

        def go(self, cond, s, which, dev_sp):
            if which == "side" and not self.side:
                return
            sem = self.side_sem if which == "side" else self.main_sem
            ref = self.part(s, which)
            send(cond, ref, ref, sem.at[s], (dev_sp, t))

        def across(self, cond, s, which):
            for d in range(1, cols):
                self.go(cond, s, which, z * cols + (x + d) % cols)

        def peers(self, level):
            return [level * cols + (x + cols - d) % cols for d in range(1, cols)]

        def begin(self):
            self.across(None, me, "side")
            self.go(up, me, "all", me + cols)
            self.go(down, me, "all", me - cols)
            self.across(None, me, "main")

        def begin_side(self):
            for s in self.peers(z) if self.side else []:
                arrived(None, self.part(s, "side"), self.side_sem.at[s])
                self.go(up, s, "side", me + cols)
                self.go(down, s, "side", me - cols)

        def hop(self, h):
            for level, there, on, to in (
                (z - h, z - h >= 0, up, me + cols),
                (z + h, z + h < levels, down, me - cols),
            ):
                s = level * cols + x
                arrived(there, self.part(s, "all"), self.main_sem.at[s])
                self.go(both(there, on), s, "all", to)
                self.across(there, s, "main")
                for s in self.peers(level) if self.side else []:
                    arrived(there, self.part(s, "side"), self.side_sem.at[s])
                    self.go(both(there, on), s, "side", to)

        def ready(self, h):
            found = []
            for level, there in (
                ((z, None),) if h == 0 else ((z - h, z - h >= 0), (z + h, z + h < levels))
            ):
                found.append((there, level * cols + x, None))
                for s in self.peers(level):
                    found.append(
                        (
                            there,
                            s,
                            functools.partial(
                                arrived, None, self.part(s, "main"), self.main_sem.at[s]
                            ),
                        )
                    )
            return found

    spread_q = Spread(wq, sem_q, None)
    spread_p = Spread(wp, sem_p, sem_p_side)
    spread_out = Spread(wo, sem_out, sem_out_side)
    for copy in locals_[:n_in]:
        copy.wait()
    spread_q.begin()
    spread_p.begin()
    tok_copy.wait()

    mine = pl.ds(pl.multiple_of(t * rows, rows), rows)
    wide = tokv[...].astype(F32)
    inverse = lax.rsqrt(jnp.mean(wide * wide, axis=1, keepdims=True) + EPS)
    for i in range(n_sp):
        span = slice(i * piece, (i + 1) * piece)
        xs[i, mine, :] = (tokv[:, span].astype(F32) * inverse * gain[:, span]).astype(BF16)

    def rows_of(device):
        return xs.at[:, pl.ds(pl.multiple_of(device * rows, rows), rows), :]

    for d in range(1, chips):
        send(None, rows_of(t), rows_of(t), sem_tok.at[t], (me, (y + d) % chips * CORES + c))
    send(None, rows_of(t), rows_of(t), sem_tok.at[t], (me, partner))

    for h in range(1, levels - 1):
        spread_q.hop(h)
    spread_p.begin_side()
    for h in range(1, levels - 2):
        spread_p.hop(h)

    for d in range(1, chips):
        far = (y + chips - d) % chips * CORES + c
        arrived(None, rows_of(far), sem_tok.at[far])
        send(None, rows_of(far), rows_of(far), sem_tok.at[far], (me, partner))
    arrived(None, rows_of(partner), sem_tok.at[partner])
    for d in range(1, chips):
        far = (y + chips - d) % chips * CORES + (1 - c)
        arrived(None, rows_of(far), sem_tok.at[far])

    spread_q.hop(levels - 1)
    for h in range(max(1, levels - 2), levels - 1):
        spread_p.hop(h)
    for copy in locals_[n_in:]:
        copy.wait()
    spread_out.begin()

    tile = row_tile(seq, 256)

    def project(spread, acc, h):
        for i, (cond, s, wait) in enumerate(spread.ready(h)):

            def run(s=s, wait=wait, first=(h == 0 and i == 0)):
                if wait is not None:
                    wait()

                @pl.loop(0, seq // tile)
                def _(i):
                    r = pl.ds(pl.multiple_of(i * tile, tile), tile)
                    value = jnp.dot(xs[s, r, :], spread.buf[s], preferred_element_type=F32)
                    if first:
                        acc[r, :] = value
                    else:
                        acc[r, :] += value

            when(cond, run)

    def settle(acc, at):
        @pl.loop(0, seq // tile)
        def _(i):
            r = pl.multiple_of(i * tile, tile)
            to = pl.ds(pl.multiple_of(r + WINDOW, WINDOW), tile)
            ext[to, at : at + acc.shape[1]] = acc[pl.ds(r, tile), :].astype(BF16)

    later, earlier = me + 1 < n_sp, me > 0

    def pass_on(at, width, i):
        head = ext.at[pl.ds(0, WINDOW), pl.ds(at, width)]
        tail = ext.at[pl.ds(seq, WINDOW), pl.ds(at, width)]
        send(later, tail, head, sem_halo.at[i], (me + 1, t))
        return head

    for h in range(levels - 1):
        project(spread_q, accq, h)
    spread_p.hop(levels - 1)
    project(spread_q, accq, levels - 1)
    settle(accq, 0)
    head_kv = pass_on(qw, kw + vw, 0)
    channel0 = qkv
    group = t * pw // POOL_CH
    whole_prefix = group == POOL_GROUPS - 1

    group_heads = qw // kw
    stacked = group_heads * WINDOW
    scale = HEAD_DIM ** (-0.5)

    def attend(n):
        q_rows = pl.ds(pl.multiple_of(n * WINDOW + WINDOW, WINDOW), WINDOW)
        k_rows = pl.ds(pl.multiple_of(n * WINDOW, WINDOW), 2 * WINDOW)
        queries = ext[q_rows, :qw]
        keys = ext[k_rows, qw : qw + kw]
        values = ext[k_rows, qw + kw : channel0]
        row = lax.broadcasted_iota(jnp.int32, (stacked, 2 * WINDOW), 0)
        q_index = row % WINDOW
        k_index = lax.broadcasted_iota(jnp.int32, (stacked, 2 * WINDOW), 1)
        lowest = jnp.where(me * blocks + n == 0, WINDOW, 0)
        allowed = (k_index > q_index) & (k_index <= q_index + WINDOW) & (k_index >= lowest)
        which = lax.broadcasted_iota(jnp.int32, (stacked, 1), 0) // WINDOW
        done = []
        for j in range(kw // HEAD_DIM):
            part = slice(j * HEAD_DIM, (j + 1) * HEAD_DIM)
            first = j * group_heads
            q = jnp.concatenate(
                [
                    queries[:, (first + g) * HEAD_DIM : (first + g + 1) * HEAD_DIM]
                    for g in range(group_heads)
                ],
                axis=0,
            )
            scores = (
                lax.dot_general(
                    q, keys[:, part], (((1,), (1,)), ((), ())), preferred_element_type=F32
                )
                * scale
            )
            scores = jnp.where(allowed, scores, -jnp.inf)
            sinks = jnp.full((stacked, 1), sink[first], F32)
            for g in range(1, group_heads):
                sinks = jnp.where(which == g, sink[first + g], sinks)
            peak = jnp.maximum(jnp.max(scores, axis=1, keepdims=True), sinks)
            expo = jnp.exp(scores - peak)
            denom = jnp.sum(expo, axis=1, keepdims=True) + jnp.exp(sinks - peak)
            probs = (expo * (1.0 / denom)).astype(BF16)
            got = jnp.dot(probs, values[:, part], preferred_element_type=F32)
            done += [got[g * WINDOW : (g + 1) * WINDOW] for g in range(group_heads)]
        to = pl.ds(pl.multiple_of(n * WINDOW, WINDOW), WINDOW)
        mix[to, :qw] = jnp.concatenate(done, axis=1).astype(BF16)

    spread_out.begin_side()
    spread_out.hop(1)
    third = max(2, (blocks + 1) // 2)
    pl.loop(1, third)(attend)
    for h in range(levels):
        project(spread_p, accp, h)
    settle(accp, channel0)
    head_pool = pass_on(channel0, pw, 1)
    total = jnp.sum(ext[WINDOW:, channel0:].astype(F32), axis=0, keepdims=True)
    tot[me] = jnp.broadcast_to(total, tot.shape[1:])
    for d in range(1, n_sp):
        send(
            both(whole_prefix, me + d < n_sp), tot.at[me], tot.at[me], sem_tot.at[me],
            (me + d, t),
        )
    pl.loop(third, blocks)(attend)

    @pl.when(jnp.logical_not(earlier))
    def _():
        ext[:WINDOW, qw:] = jnp.zeros((WINDOW, ext.shape[1] - qw), BF16)

    arrived(earlier, head_kv, sem_halo.at[0])
    attend(0)
    for h in range(2, levels - 1):
        spread_out.hop(h)
    arrived(earlier, head_pool, sem_halo.at[1])

    carry[...] = jnp.zeros(carry.shape, F32)
    for d in range(1, n_sp):

        def add(d=d):
            arrived(None, tot.at[me - d], sem_tot.at[me - d])
            carry[...] += tot[me - d]

        when(both(whole_prefix, me - d >= 0), add)

    reach = jnp.where(
        group == 0, SHORT_REACHES[0], jnp.where(group == 1, SHORT_REACHES[1], WINDOW)
    )
    reach = jnp.where(whole_prefix, n_sp * seq, reach)
    lowest = jnp.where(whole_prefix, WINDOW, 0)

    @pl.loop(0, blocks)
    def _(n):
        q_index = lax.broadcasted_iota(jnp.int32, (WINDOW, 2 * WINDOW), 0)
        k_index = lax.broadcasted_iota(jnp.int32, (WINDOW, 2 * WINDOW), 1)
        distance = q_index + WINDOW - k_index
        band = (distance >= 0) & (distance < reach) & (k_index >= lowest)
        band = jnp.where(band, 1.0, 0.0).astype(BF16)
        k_rows = pl.ds(pl.multiple_of(n * WINDOW, WINDOW), 2 * WINDOW)
        both_blocks = ext[k_rows, channel0:]
        sums = jnp.dot(band, both_blocks, preferred_element_type=F32) + carry[0:1, :]
        position = me * seq + n * WINDOW + lax.broadcasted_iota(jnp.int32, (WINDOW, 1), 0)
        counted = jnp.minimum(position + 1, reach).astype(F32)
        mixed = (sums / counted - both_blocks[WINDOW:].astype(F32)) * pgain[...]
        mix[pl.ds(pl.multiple_of(n * WINDOW, WINDOW), WINDOW), qw:] = mixed.astype(BF16)
        carry[...] = jnp.where(
            whole_prefix, jnp.broadcast_to(sums[WINDOW - 1 :], carry.shape), 0.0
        )

    def mix_rows(chip, core):
        return mix[pl.ds(pl.multiple_of((chip * CORES + core) * rows, rows), rows), :]

    outs = []

    def multiply(cond, s, wait):
        def run():
            if wait is not None:
                wait()
            for chip in range(chips):
                dsend[s, chip] = jnp.dot(
                    mix_rows(chip, 1 - c), wo[s], preferred_element_type=F32
                ).astype(BF16)

        when(cond, run)
        send(cond, dsend.at[s], drecv.at[s], sem_core.at[s], (me, partner))

        def keep():
            for chip in range(chips):
                own[s, chip] = jnp.dot(mix_rows(chip, c), wo[s], preferred_element_type=F32)

        when(cond, keep)

    def finish(cond, s):
        arrived(cond, drecv.at[s], sem_core.at[s])
        for d in range(1, chips):
            far = (y + d) % chips

            def pack(d=d, far=far):
                ysend[s, d - 1] = (own[s, far] + drecv[s, far].astype(F32)).astype(BF16)

            when(cond, pack)
            last.append(len(sent))
            send(
                cond, ysend.at[s, d - 1], yrecv.at[s, d - 1], sem_y.at[s, d - 1],
                (me, far * CORES + c),
            )

    last = []
    pending = None
    for h in range(levels):
        if h == levels - 1:
            if pending is not None:
                finish(*pending)
                pending = None
            spread_out.hop(h)
        for cond, s, wait in spread_out.ready(h):
            multiply(cond, s, wait)
            if pending is not None:
                finish(*pending)
            pending = (cond, s)
    finish(*pending)

    for i, (cond, copy) in enumerate(sent):
        if i not in last:
            when(cond, copy.wait_send)

    for i in range(n_sp):
        value = own[i, y] + drecv[i, y].astype(F32)
        for d in range(1, chips):
            arrived(None, yrecv.at[i, d - 1], sem_y.at[i, d - 1])
            value += yrecv[i, d - 1].astype(F32)
        w = wo.shape[2]
        out[:, i * w : (i + 1) * w] = value.astype(BF16)

    for i in last:
        when(sent[i][0], sent[i][1].wait_send)


def local(
    n_sp, n_tp, tokens_in, norm_gain, query_weight, key_weight, value_weight, pool_weight,
    sink_logit, pool_gain, attention_out_weight, pool_out_weight,
):
    rows, depth = tokens_in.shape
    seq = rows * n_tp
    ins = [query_weight, key_weight, value_weight, pool_weight]
    outs = [attention_out_weight, pool_out_weight]
    widths = tuple(w.shape[1] for w in ins)
    if any(w % 128 for w in widths):
        ins = [jnp.concatenate(ins[:3], axis=1), ins[3]]
    cols = math.gcd(n_sp, max(1, n_tp // CORES))
    levels, chips = n_sp // cols, n_tp // CORES
    k_in, k_out = ins[0].shape[0], sum(w.shape[0] for w in outs)
    width, out_cols = sum(widths), outs[0].shape[1]
    pw = widths[3]
    hops = 2 * (levels - 1) + 1
    n_send = 3 * (2 + 2 * cols + hops * (2 + 3 * cols)) + 2 * n_tp + n_sp + 2
    n_send += 2 * n_sp * hops * chips
    vmem = pl.BlockSpec(memory_space=pltpu.VMEM)
    hbm = pl.BlockSpec(memory_space=pl.ANY)
    dma = pltpu.SemaphoreType.DMA
    return pl.pallas_call(
        functools.partial(kernel, n_sp, n_tp, cols, len(ins), len(outs), widths),
        out_shape=jax.ShapeDtypeStruct((rows, depth), BF16),
        in_specs=[hbm, vmem, pl.BlockSpec(memory_space=pltpu.SMEM), vmem]
        + [hbm] * (len(ins) + len(outs)),
        out_specs=vmem,
        scratch_shapes=[
            pltpu.VMEM((rows, depth), BF16),
            pltpu.VMEM((n_sp, seq, depth // n_sp), BF16),
            pltpu.VMEM((n_sp, k_in, width - pw), BF16),
            pltpu.VMEM((n_sp, k_in, pw), BF16),
            pltpu.VMEM((n_sp, k_out, out_cols), BF16),
            pltpu.VMEM((seq, width - pw), F32),
            pltpu.VMEM((seq, pw), F32),
            pltpu.VMEM((seq + WINDOW, width), BF16),
            pltpu.VMEM((seq, widths[0] + pw), BF16),
            pltpu.VMEM((n_sp, 8, pw), F32),
            pltpu.VMEM((8, pw), F32),
            pltpu.VMEM((n_sp, chips, rows, out_cols), BF16),
            pltpu.VMEM((n_sp, chips, rows, out_cols), BF16),
            pltpu.VMEM((n_sp, max(1, chips - 1), rows, out_cols), BF16),
            pltpu.VMEM((n_sp, max(1, chips - 1), rows, out_cols), BF16),
            pltpu.VMEM((n_sp, chips, rows, out_cols), F32),
            dma((len(ins) + len(outs) + 1,)),
            dma((n_send,)),
            dma((n_sp,)),
            dma((n_sp,)),
            dma((n_sp,)),
            dma((n_sp,)),
            dma((n_sp,)),
            dma((n_tp,)),
            dma((2,)),
            dma((n_sp,)),
            dma((n_sp,)),
            dma((n_sp, max(1, chips - 1))),
        ],
        compiler_params=pltpu.CompilerParams(
            collective_id=0, has_side_effects=True, vmem_limit_bytes=58 << 20
        ),
    )(
        tokens_in, norm_gain.reshape(1, -1), sink_logit, pool_gain.reshape(1, -1), *ins, *outs
    )


def solution(mesh):
    in_specs = (
        P(("sp", "tp"), None), P(), P("sp", "tp"), P("sp", "tp"), P("sp", "tp"), P("sp", "tp"),
        P("tp"), P("tp"), P("tp", "sp"), P("tp", "sp"),
    )
    out_specs = P(("sp", "tp"), None)
    return jax.shard_map(
        functools.partial(local, mesh.shape["sp"], mesh.shape["tp"]),
        mesh=mesh, in_specs=in_specs, out_specs=out_specs, check_vma=False,
    )
```

```python
import functools
import math

import jax
import jax.numpy as jnp
from jax import lax
from jax.experimental import pallas as pl
from jax.experimental.pallas import tpu as pltpu
from jax.sharding import PartitionSpec as P

HEAD_DIM = 64
POOL_CH = 256
POOL_GROUPS = 4
WINDOW = 128
EPS = 1e-06
SHORT_REACHES = (8, 32)
CORES = 2
SIDE_SHARE = 0.3
MESH = pl.DeviceIdType.MESH
F32 = jnp.float32
BF16 = jnp.bfloat16


def row_tile(rows, most):
    tile = most
    while rows % tile:
        tile -= 16
    return tile


def kernel(n_sp, n_tp, cols, n_in, n_out, widths, *refs):
    tok, gain, sink, pgain = refs[:4]
    win_refs = refs[4 : 4 + n_in]
    wout_refs = refs[4 + n_in : 4 + n_in + n_out]
    (
        out, tokv, xs, wq, wp, wo, accq, accp, ext, mix, tot, carry, dsend, drecv, ysend, yrecv, own,
        local_sem, send_sem, sem_q, sem_p, sem_p_side, sem_out, sem_out_side,
        sem_tok, sem_halo, sem_tot, sem_core, sem_y,
    ) = refs[4 + n_in + n_out :]
    qw, kw, vw, pw = widths
    levels = n_sp // cols
    chips = n_tp // CORES
    rows, seq = tok.shape[0], xs.shape[1]
    qkv = wq.shape[2]
    piece = xs.shape[2]
    blocks = seq // WINDOW
    me, t = lax.axis_index("sp"), lax.axis_index("tp")
    z, x = me // cols, me % cols
    y, c = t // CORES, t % CORES
    partner = y * CORES + (1 - c)

    locals_ = []
    at = 0
    for i, ref in enumerate(win_refs[:-1]):
        w = ref.shape[1]
        locals_.append(pltpu.make_async_copy(ref, wq.at[me, :, pl.ds(at, w)], local_sem.at[i]))
        at += w
    locals_.append(pltpu.make_async_copy(win_refs[-1], wp.at[me], local_sem.at[n_in - 1]))
    at = 0
    for i, ref in enumerate(wout_refs):
        k = ref.shape[0]
        locals_.append(
            pltpu.make_async_copy(ref, wo.at[me, pl.ds(at, k), :], local_sem.at[n_in + i])
        )
        at += k
    tok_copy = pltpu.make_async_copy(tok, tokv, local_sem.at[n_in + n_out])
    for copy in locals_[:n_in] + [tok_copy] + locals_[n_in:]:
        copy.start()

    barrier = pltpu.get_barrier_semaphore()
    for d in range(1, n_sp):
        pl.semaphore_signal(barrier, inc=1, device_id=((me + d) % n_sp, t), device_id_type=MESH)
    for d in range(1, n_tp):
        pl.semaphore_signal(barrier, inc=1, device_id=(me, (t + d) % n_tp), device_id_type=MESH)
    pl.semaphore_wait(barrier, n_sp + n_tp - 2)

    sent = []

    def when(cond, fn):
        if cond is None:
            fn()
        else:
            pl.when(cond)(fn)

    def both(a, b):
        return b if a is None else (a if b is None else jnp.logical_and(a, b))

    def send(cond, src, dst, recv, dev):
        copy = pltpu.make_async_remote_copy(
            src_ref=src, dst_ref=dst, send_sem=send_sem.at[len(sent)], recv_sem=recv,
            device_id=dev, device_id_type=MESH,
        )
        when(cond, copy.start)
        sent.append((cond, copy))

    def arrived(cond, dst, recv):
        copy = pltpu.make_async_remote_copy(
            src_ref=dst, dst_ref=dst, send_sem=send_sem.at[0], recv_sem=recv,
            device_id=(me, partner), device_id_type=MESH,
        )
        when(cond, copy.wait_recv)

    up, down = z + 1 < levels, z > 0

    class Spread:
        def __init__(self, buf, main_sem, side_sem):
            self.buf, self.main_sem, self.side_sem = buf, main_sem, side_sem
            k = buf.shape[1]
            self.side = 0 if side_sem is None else max(16, int(k * SIDE_SHARE) // 16 * 16)
            self.main = k - self.side

        def part(self, s, which):
            if which == "all":
                return self.buf.at[s]
            if which == "main":
                return self.buf.at[s, pl.ds(0, self.main), :]
            return self.buf.at[s, pl.ds(self.main, self.side), :]

        def go(self, cond, s, which, dev_sp):
            if which == "side" and not self.side:
                return
            sem = self.side_sem if which == "side" else self.main_sem
            ref = self.part(s, which)
            send(cond, ref, ref, sem.at[s], (dev_sp, t))

        def across(self, cond, s, which):
            for d in range(1, cols):
                self.go(cond, s, which, z * cols + (x + d) % cols)

        def peers(self, level):
            return [level * cols + (x + cols - d) % cols for d in range(1, cols)]

        def begin(self):
            self.across(None, me, "side")
            self.go(up, me, "all", me + cols)
            self.go(down, me, "all", me - cols)
            self.across(None, me, "main")

        def begin_side(self):
            for s in self.peers(z) if self.side else []:
                arrived(None, self.part(s, "side"), self.side_sem.at[s])
                self.go(up, s, "side", me + cols)
                self.go(down, s, "side", me - cols)

        def ways(self, h):
            return (
                (z - h, z - h >= 0, up, me + cols),
                (z + h, z + h < levels, down, me - cols),
            )

        def hop_main(self, h):
            for level, there, on, to in self.ways(h):
                s = level * cols + x
                arrived(there, self.part(s, "all"), self.main_sem.at[s])
                self.go(both(there, on), s, "all", to)
                self.across(there, s, "main")

        def hop_side(self, h):
            for level, there, on, to in self.ways(h) if self.side else ():
                for s in self.peers(level):
                    arrived(there, self.part(s, "side"), self.side_sem.at[s])
                    self.go(both(there, on), s, "side", to)

        def hop(self, h):
            self.hop_main(h)
            self.hop_side(h)

        def ready(self, h):
            found = []
            for level, there in (
                ((z, None),) if h == 0 else ((z - h, z - h >= 0), (z + h, z + h < levels))
            ):
                found.append((there, level * cols + x, None))
                for s in self.peers(level):
                    found.append(
                        (
                            there,
                            s,
                            functools.partial(
                                arrived, None, self.part(s, "main"), self.main_sem.at[s]
                            ),
                        )
                    )
            return found

    spread_q = Spread(wq, sem_q, None)
    spread_p = Spread(wp, sem_p, sem_p_side)
    spread_out = Spread(wo, sem_out, sem_out_side)
    for copy in locals_[:n_in]:
        copy.wait()
    spread_q.begin()
    spread_p.begin()
    tok_copy.wait()

    mine = pl.ds(pl.multiple_of(t * rows, rows), rows)
    wide = tokv[...].astype(F32)
    inverse = lax.rsqrt(jnp.mean(wide * wide, axis=1, keepdims=True) + EPS)
    for i in range(n_sp):
        span = slice(i * piece, (i + 1) * piece)
        xs[i, mine, :] = (tokv[:, span].astype(F32) * inverse * gain[:, span]).astype(BF16)

    def rows_of(device):
        return xs.at[:, pl.ds(pl.multiple_of(device * rows, rows), rows), :]

    for d in range(1, chips):
        send(None, rows_of(t), rows_of(t), sem_tok.at[t], (me, (y + d) % chips * CORES + c))
    send(None, rows_of(t), rows_of(t), sem_tok.at[t], (me, partner))

    for h in range(1, levels - 1):
        spread_q.hop(h)
    spread_p.begin_side()
    for h in range(1, levels - 2):
        spread_p.hop(h)

    for d in range(1, chips):
        far = (y + chips - d) % chips * CORES + c
        arrived(None, rows_of(far), sem_tok.at[far])
        send(None, rows_of(far), rows_of(far), sem_tok.at[far], (me, partner))
    arrived(None, rows_of(partner), sem_tok.at[partner])
    for d in range(1, chips):
        far = (y + chips - d) % chips * CORES + (1 - c)
        arrived(None, rows_of(far), sem_tok.at[far])

    spread_q.hop(levels - 1)
    for h in range(max(1, levels - 2), levels - 1):
        spread_p.hop(h)
    for copy in locals_[n_in:]:
        copy.wait()
    spread_out.begin()

    tile = row_tile(seq, 256)

    def project(spread, acc, h):
        for i, (cond, s, wait) in enumerate(spread.ready(h)):

            def run(s=s, wait=wait, first=(h == 0 and i == 0)):
                if wait is not None:
                    wait()

                @pl.loop(0, seq // tile)
                def _(i):
                    r = pl.ds(pl.multiple_of(i * tile, tile), tile)
                    value = jnp.dot(xs[s, r, :], spread.buf[s], preferred_element_type=F32)
                    if first:
                        acc[r, :] = value
                    else:
                        acc[r, :] += value

            when(cond, run)

    def settle(acc, at):
        @pl.loop(0, seq // tile)
        def _(i):
            r = pl.multiple_of(i * tile, tile)
            to = pl.ds(pl.multiple_of(r + WINDOW, WINDOW), tile)
            ext[to, at : at + acc.shape[1]] = acc[pl.ds(r, tile), :].astype(BF16)

    later, earlier = me + 1 < n_sp, me > 0

    def pass_on(at, width, i):
        head = ext.at[pl.ds(0, WINDOW), pl.ds(at, width)]
        tail = ext.at[pl.ds(seq, WINDOW), pl.ds(at, width)]
        send(later, tail, head, sem_halo.at[i], (me + 1, t))
        return head

    for h in range(levels - 1):
        project(spread_q, accq, h)
    spread_p.hop(levels - 1)
    project(spread_q, accq, levels - 1)
    settle(accq, 0)
    head_kv = pass_on(qw, kw + vw, 0)
    channel0 = qkv
    group = t * pw // POOL_CH
    whole_prefix = group == POOL_GROUPS - 1

    group_heads = qw // kw
    stacked = group_heads * WINDOW
    scale = HEAD_DIM ** (-0.5)

    def attend(n):
        q_rows = pl.ds(pl.multiple_of(n * WINDOW + WINDOW, WINDOW), WINDOW)
        k_rows = pl.ds(pl.multiple_of(n * WINDOW, WINDOW), 2 * WINDOW)
        queries = ext[q_rows, :qw]
        keys = ext[k_rows, qw : qw + kw]
        values = ext[k_rows, qw + kw : channel0]
        row = lax.broadcasted_iota(jnp.int32, (stacked, 2 * WINDOW), 0)
        q_index = row % WINDOW
        k_index = lax.broadcasted_iota(jnp.int32, (stacked, 2 * WINDOW), 1)
        lowest = jnp.where(me * blocks + n == 0, WINDOW, 0)
        allowed = (k_index > q_index) & (k_index <= q_index + WINDOW) & (k_index >= lowest)
        which = lax.broadcasted_iota(jnp.int32, (stacked, 1), 0) // WINDOW
        done = []
        for j in range(kw // HEAD_DIM):
            part = slice(j * HEAD_DIM, (j + 1) * HEAD_DIM)
            first = j * group_heads
            q = jnp.concatenate(
                [
                    queries[:, (first + g) * HEAD_DIM : (first + g + 1) * HEAD_DIM]
                    for g in range(group_heads)
                ],
                axis=0,
            )
            scores = (
                lax.dot_general(
                    q, keys[:, part], (((1,), (1,)), ((), ())), preferred_element_type=F32
                )
                * scale
            )
            scores = jnp.where(allowed, scores, -jnp.inf)
            sinks = jnp.full((stacked, 1), sink[first], F32)
            for g in range(1, group_heads):
                sinks = jnp.where(which == g, sink[first + g], sinks)
            peak = jnp.maximum(jnp.max(scores, axis=1, keepdims=True), sinks)
            expo = jnp.exp(scores - peak)
            denom = jnp.sum(expo, axis=1, keepdims=True) + jnp.exp(sinks - peak)
            probs = (expo * (1.0 / denom)).astype(BF16)
            got = jnp.dot(probs, values[:, part], preferred_element_type=F32)
            done += [got[g * WINDOW : (g + 1) * WINDOW] for g in range(group_heads)]
        to = pl.ds(pl.multiple_of(n * WINDOW, WINDOW), WINDOW)
        mix[to, :qw] = jnp.concatenate(done, axis=1).astype(BF16)

    third = max(2, (blocks + 1) // 2)
    pl.loop(1, third)(attend)
    spread_out.hop_main(1)
    pl.loop(third, blocks)(attend)
    for h in range(levels):
        project(spread_p, accp, h)
    settle(accp, channel0)
    head_pool = pass_on(channel0, pw, 1)
    total = jnp.sum(ext[WINDOW:, channel0:].astype(F32), axis=0, keepdims=True)
    tot[me] = jnp.broadcast_to(total, tot.shape[1:])
    for d in range(1, n_sp):
        send(
            both(whole_prefix, me + d < n_sp), tot.at[me], tot.at[me], sem_tot.at[me],
            (me + d, t),
        )
    for h in range(2, levels - 1):
        spread_out.hop_main(h)
    spread_out.begin_side()
    spread_out.hop_side(1)

    @pl.when(jnp.logical_not(earlier))
    def _():
        ext[:WINDOW, qw:] = jnp.zeros((WINDOW, ext.shape[1] - qw), BF16)

    arrived(earlier, head_kv, sem_halo.at[0])
    attend(0)
    for h in range(2, levels - 1):
        spread_out.hop_side(h)
    arrived(earlier, head_pool, sem_halo.at[1])

    carry[...] = jnp.zeros(carry.shape, F32)
    for d in range(1, n_sp):

        def add(d=d):
            arrived(None, tot.at[me - d], sem_tot.at[me - d])
            carry[...] += tot[me - d]

        when(both(whole_prefix, me - d >= 0), add)

    reach = jnp.where(
        group == 0, SHORT_REACHES[0], jnp.where(group == 1, SHORT_REACHES[1], WINDOW)
    )
    reach = jnp.where(whole_prefix, n_sp * seq, reach)
    lowest = jnp.where(whole_prefix, WINDOW, 0)

    @pl.loop(0, blocks)
    def _(n):
        q_index = lax.broadcasted_iota(jnp.int32, (WINDOW, 2 * WINDOW), 0)
        k_index = lax.broadcasted_iota(jnp.int32, (WINDOW, 2 * WINDOW), 1)
        distance = q_index + WINDOW - k_index
        band = (distance >= 0) & (distance < reach) & (k_index >= lowest)
        band = jnp.where(band, 1.0, 0.0).astype(BF16)
        k_rows = pl.ds(pl.multiple_of(n * WINDOW, WINDOW), 2 * WINDOW)
        both_blocks = ext[k_rows, channel0:]
        sums = jnp.dot(band, both_blocks, preferred_element_type=F32) + carry[0:1, :]
        position = me * seq + n * WINDOW + lax.broadcasted_iota(jnp.int32, (WINDOW, 1), 0)
        counted = jnp.minimum(position + 1, reach).astype(F32)
        mixed = (sums / counted - both_blocks[WINDOW:].astype(F32)) * pgain[...]
        mix[pl.ds(pl.multiple_of(n * WINDOW, WINDOW), WINDOW), qw:] = mixed.astype(BF16)
        carry[...] = jnp.where(
            whole_prefix, jnp.broadcast_to(sums[WINDOW - 1 :], carry.shape), 0.0
        )

    def mix_rows(chip, core):
        return mix[pl.ds(pl.multiple_of((chip * CORES + core) * rows, rows), rows), :]

    outs = []

    def multiply(cond, s, wait):
        def run():
            if wait is not None:
                wait()
            for chip in range(chips):
                dsend[s, chip] = jnp.dot(
                    mix_rows(chip, 1 - c), wo[s], preferred_element_type=F32
                ).astype(BF16)

        when(cond, run)
        send(cond, dsend.at[s], drecv.at[s], sem_core.at[s], (me, partner))

        def keep():
            for chip in range(chips):
                own[s, chip] = jnp.dot(mix_rows(chip, c), wo[s], preferred_element_type=F32)

        when(cond, keep)

    def finish(cond, s):
        arrived(cond, drecv.at[s], sem_core.at[s])
        for d in range(1, chips):
            far = (y + d) % chips

            def pack(d=d, far=far):
                ysend[s, d - 1] = (own[s, far] + drecv[s, far].astype(F32)).astype(BF16)

            when(cond, pack)
            last.append(len(sent))
            send(
                cond, ysend.at[s, d - 1], yrecv.at[s, d - 1], sem_y.at[s, d - 1],
                (me, far * CORES + c),
            )

    last = []
    pending = None
    for h in range(levels):
        if h == levels - 1:
            if pending is not None:
                finish(*pending)
                pending = None
            spread_out.hop(h)
        for cond, s, wait in spread_out.ready(h):
            multiply(cond, s, wait)
            if pending is not None:
                finish(*pending)
            pending = (cond, s)
    finish(*pending)

    for i, (cond, copy) in enumerate(sent):
        if i not in last:
            when(cond, copy.wait_send)

    for i in range(n_sp):
        value = own[i, y] + drecv[i, y].astype(F32)
        for d in range(1, chips):
            arrived(None, yrecv.at[i, d - 1], sem_y.at[i, d - 1])
            value += yrecv[i, d - 1].astype(F32)
        w = wo.shape[2]
        out[:, i * w : (i + 1) * w] = value.astype(BF16)

    for i in last:
        when(sent[i][0], sent[i][1].wait_send)


def local(
    n_sp, n_tp, tokens_in, norm_gain, query_weight, key_weight, value_weight, pool_weight,
    sink_logit, pool_gain, attention_out_weight, pool_out_weight,
):
    rows, depth = tokens_in.shape
    seq = rows * n_tp
    ins = [query_weight, key_weight, value_weight, pool_weight]
    outs = [attention_out_weight, pool_out_weight]
    widths = tuple(w.shape[1] for w in ins)
    if any(w % 128 for w in widths):
        ins = [jnp.concatenate(ins[:3], axis=1), ins[3]]
    cols = math.gcd(n_sp, max(1, n_tp // CORES))
    levels, chips = n_sp // cols, n_tp // CORES
    k_in, k_out = ins[0].shape[0], sum(w.shape[0] for w in outs)
    width, out_cols = sum(widths), outs[0].shape[1]
    pw = widths[3]
    hops = 2 * (levels - 1) + 1
    n_send = 3 * (2 + 2 * cols + hops * (2 + 3 * cols)) + 2 * n_tp + n_sp + 2
    n_send += 2 * n_sp * hops * chips
    vmem = pl.BlockSpec(memory_space=pltpu.VMEM)
    hbm = pl.BlockSpec(memory_space=pl.ANY)
    dma = pltpu.SemaphoreType.DMA
    return pl.pallas_call(
        functools.partial(kernel, n_sp, n_tp, cols, len(ins), len(outs), widths),
        out_shape=jax.ShapeDtypeStruct((rows, depth), BF16),
        in_specs=[hbm, vmem, pl.BlockSpec(memory_space=pltpu.SMEM), vmem]
        + [hbm] * (len(ins) + len(outs)),
        out_specs=vmem,
        scratch_shapes=[
            pltpu.VMEM((rows, depth), BF16),
            pltpu.VMEM((n_sp, seq, depth // n_sp), BF16),
            pltpu.VMEM((n_sp, k_in, width - pw), BF16),
            pltpu.VMEM((n_sp, k_in, pw), BF16),
            pltpu.VMEM((n_sp, k_out, out_cols), BF16),
            pltpu.VMEM((seq, width - pw), F32),
            pltpu.VMEM((seq, pw), F32),
            pltpu.VMEM((seq + WINDOW, width), BF16),
            pltpu.VMEM((seq, widths[0] + pw), BF16),
            pltpu.VMEM((n_sp, 8, pw), F32),
            pltpu.VMEM((8, pw), F32),
            pltpu.VMEM((n_sp, chips, rows, out_cols), BF16),
            pltpu.VMEM((n_sp, chips, rows, out_cols), BF16),
            pltpu.VMEM((n_sp, max(1, chips - 1), rows, out_cols), BF16),
            pltpu.VMEM((n_sp, max(1, chips - 1), rows, out_cols), BF16),
            pltpu.VMEM((n_sp, chips, rows, out_cols), F32),
            dma((len(ins) + len(outs) + 1,)),
            dma((n_send,)),
            dma((n_sp,)),
            dma((n_sp,)),
            dma((n_sp,)),
            dma((n_sp,)),
            dma((n_sp,)),
            dma((n_tp,)),
            dma((2,)),
            dma((n_sp,)),
            dma((n_sp,)),
            dma((n_sp, max(1, chips - 1))),
        ],
        compiler_params=pltpu.CompilerParams(
            collective_id=0, has_side_effects=True, vmem_limit_bytes=58 << 20
        ),
    )(
        tokens_in, norm_gain.reshape(1, -1), sink_logit, pool_gain.reshape(1, -1), *ins, *outs
    )


def solution(mesh):
    in_specs = (
        P(("sp", "tp"), None), P(), P("sp", "tp"), P("sp", "tp"), P("sp", "tp"), P("sp", "tp"),
        P("tp"), P("tp"), P("tp", "sp"), P("tp", "sp"),
    )
    out_specs = P(("sp", "tp"), None)
    return jax.shard_map(
        functools.partial(local, mesh.shape["sp"], mesh.shape["tp"]),
        mesh=mesh, in_specs=in_specs, out_specs=out_specs, check_vma=False,
    )
```
